32 devices in a mesh: grp: 2 (over x), ep: 16 (over z, y, core).
Axes of the slice: x: 2, y: 2, z: 4, core: 2. Of those that a mesh axis runs over, the one named last changes fastest.
Arguments:
- tokens: bfloat16 [128, 2048], P(('grp', 'ep')), parts along dimension 0, may hold values from -30 to 30
- state: float32 [128, 16, 128, 128], P(('grp', 'ep')), parts along dimension 0, may hold values from -6 to 6
- route_ids: int32 [128, 2], P(('grp', 'ep')), parts along dimension 0, may hold values from 0 to 3, all different within a row; in each aligned block of 4 rows (0 to 3, 4 to 7, ...) at most 3 rows name the same one
- route_weights: bfloat16 [128, 2], P(('grp', 'ep')), parts along dimension 0, may hold values from 0.099609375 to 1
- norm_mix: float32 [2048], replicated, may hold values from 0.1 to 1.9
- w_query: bfloat16 [2048, 2048], P(None, 'ep'), may hold values from -0.125 to 0.125
- w_forget: bfloat16 [2048, 2048], P(None, 'ep'), may hold values from -0.125 to 0.125
- w_input: bfloat16 [2048, 2048], P(None, 'ep'), may hold values from -0.125 to 0.125
- w_gate: bfloat16 [2048, 2048], P(None, 'ep'), may hold values from -0.125 to 0.125
- lower_bound: float32 [2048], replicated, may hold values from 0.05 to 0.9
- head_gain: float32 [128], replicated, may hold values from 0.1 to 1.9
- w_out: bfloat16 [2048, 2048], P(None, 'ep'), may hold values from -0.125 to 0.125
- norm_ffn: float32 [2048], replicated, may hold values from 0.1 to 1.9
- expert_gate: bfloat16 [2048, 28672], P(None, 'ep'), may hold values from -0.125 to 0.125
- expert_up: bfloat16 [2048, 28672], P(None, 'ep'), may hold values from -0.125 to 0.125
- expert_down: bfloat16 [28672, 2048], P('ep'), may hold values from -0.0625 to 0.0625
Outputs:
- layer_out: bfloat16 [128, 2048], P(('grp', 'ep')), parts along dimension 0
- new_state: float32 [128, 16, 128, 128], P(('grp', 'ep')), parts along dimension 0
The draws below stay inside these ranges and needn't reach their ends.
There are 2 independent parts, one for each index of `grp`. The reference program is written for one: setup_inputs(seed, part) draws one part's arguments, and reference() takes and returns one part's arrays. A program takes and returns all parts, laid end to end along the dimension named above; an argument that names none is the same for every part. Nothing has to cross between parts.
Inputs may be any that keep to these rules, and one draw needn't show every extreme that they name: `route_ids`: each row names 2 different experts; the rows of one device name no expert more than 3 times, and some device names one exactly 3 times.
All inputs are finite; a program needn't handle non-finite values.
Results may differ from the reference program's by a relative error of at most 0.008.
Values may be sent and summed in bfloat16 or wider, within the bound.
No kernel may reach another device: no remote copies, remote signals or barrier semaphores. Data moves between devices by JAX's collectives and lax.ppermute only.
A program may use at most 64 MiB of HBM per device.

```python
import math
import jax
import jax.numpy as jnp
import numpy as np
from jax import lax

D = 2048
HEAD_DIM = 128
HEADS = 16
FF = 7168
EXPERTS = 4
TOP_K = 2
SEQ_DEV = 4
TOKENS = 64
CAP = 3


def draw_tokens(key, part):
    row_key, col_key, value_key = jax.random.split(key, 3)
    col_scale = jnp.exp(jnp.linspace(jnp.log(0.3), jnp.log(3.0), D))
    col_scale = col_scale * jnp.exp(jax.random.uniform(col_key, (D,), jnp.float32, -0.35, 0.35))
    row_scale = jnp.exp(jax.random.uniform(row_key, (TOKENS, 1), jnp.float32, jnp.log(0.5), jnp.log(1.5)))
    values = jax.random.normal(value_key, (TOKENS, D), jnp.float32)
    return jnp.clip(values * row_scale * col_scale[None, :], -30.0, 30.0).astype(jnp.bfloat16)


def block_scale(own_key, shape, cuts, low, top_value):
    factor_of, own = 1.0, jax.random.fold_in(own_key, 6)
    for position, shards_of in cuts:
        steps = jnp.exp(jax.random.uniform(jax.random.fold_in(own, position), (shards_of,), jnp.float32, low / len(cuts), top_value / len(cuts)))
        factor_of = factor_of * jnp.repeat(steps, shape[position] // shards_of).reshape([-1 if axis == position else 1 for axis in range(len(shape))])
    return factor_of


def assign_block(rng, own, number, rows, count, top, most, skew):
    ranking = jax.random.permutation(rng, count)
    heavy_load, ordinary = load_shares(count, rows * top, most, skew, True), load_shares(count, rows * top, most, skew, False)
    places = jnp.arange(count)

    def named(tallies, offset_by):
        used = int((tallies > 0).sum())
        fixed = max(1, used // 4)
        shifted = fixed + (places - fixed + offset_by * (used - fixed)) % max(1, count - fixed)
        return jnp.zeros((count,), jnp.int32).at[ranking[jnp.where(places < fixed, places, shifted)]].set(jnp.asarray(tallies, jnp.int32))

    tallies = jnp.where(number % 4 == 0, named(heavy_load, number // 4), named(ordinary, number - number // 4 - 1))
    mixed = jax.random.permutation(jax.random.fold_in(own, 3), count)
    giver, receiver = mixed[0:count // 2 * 2:2], mixed[1:count // 2 * 2:2]
    slack = jnp.minimum(tallies[giver] - 1, most - tallies[receiver]) // 2
    slack = jnp.where((giver == ranking[0]) | (receiver == ranking[0]) | (tallies[receiver] == 0), 0, jnp.maximum(slack, 0))
    shifted = jax.random.randint(jax.random.fold_in(own, 4), (count // 2,), 0, 1 << 20) % (slack + 1)
    tallies = tallies.at[giver].add(-shifted).at[receiver].add(shifted)
    members = jnp.searchsorted(jnp.cumsum(tallies), jnp.arange(rows * top), side="right").astype(jnp.int32)
    grid = members.reshape(top, rows).T
    grid = grid[jax.random.permutation(jax.random.fold_in(own, 1), rows)]
    offset_by = jax.random.randint(jax.random.fold_in(own, 2), (rows, 1), 0, top)
    return jnp.take_along_axis(grid, (jnp.arange(top)[None, :] + offset_by) % top, axis=1)


def load_shares(amount, total, limit, lean, full):
    weights = [(1 << 20) // math.isqrt(rank ** lean) + 1 for rank in range(1, amount + 1)]
    largest = limit if full else min(limit, max(-(-total // amount), total * weights[0] // sum(weights)))
    least = 1 if total - largest >= amount - 1 else 0
    given, spare = [largest] + [least] * (amount - 1), total - largest - least * (amount - 1)
    while spare > 0:
        movable = [i for i in range(1, amount) if given[i] < largest] or [i for i in range(1, amount) if given[i] < limit]
        pool, left = sum([weights[i] for i in movable]), spare
        for i in movable:
            extra = min(limit - given[i], max(1, left * weights[i] // pool), spare)
            given[i] = given[i] + extra
            spare = spare - extra
    return np.array(given)


def centred(own_key, dims, spread, bound, pieces=(), held_as=jnp.bfloat16):
    factor_of = block_scale(own_key, dims, pieces, -0.22, 0.18) if pieces else 1.0
    result = jax.random.normal(own_key, dims, jnp.float32) * spread * factor_of
    return jnp.minimum(jnp.maximum(result, -bound), bound).astype(held_as)


def setup_inputs(seed: int = 0, part: int = 0) -> dict:
    splits = jax.random.split(jax.random.key(seed), 17)
    part_keys = jax.random.split(jax.random.fold_in(splits[16], part), 17)
    tokens = draw_tokens(jax.random.fold_in(jax.random.fold_in(splits[16], part), 71), part)
    state = centred(part_keys[1], (TOKENS, HEADS, HEAD_DIM, HEAD_DIM), 1.0, 6.0, ((0, 16),), jnp.float32)
    route_ids_keys = jax.random.split(jax.random.fold_in(part_keys[2], 1), TOKENS // SEQ_DEV)
    route_ids_turns = jax.random.permutation(jax.random.fold_in(part_keys[2], 3), TOKENS // SEQ_DEV)
    route_ids = jax.vmap(lambda own, number: assign_block(jax.random.fold_in(part_keys[2], 2), own, number, SEQ_DEV, EXPERTS, TOP_K, CAP, 1))(route_ids_keys, route_ids_turns).reshape((TOKENS, TOP_K))
    route_weights = jnp.clip(0.099609375 + 0.9003906 * jax.random.uniform(part_keys[3], (TOKENS, TOP_K), jnp.float32) ** block_scale(part_keys[3], (TOKENS, TOP_K), ((0, 16),), -0.2, 0.2), 0.099609375, 1.0).astype(jnp.bfloat16)
    norm_mix = jnp.clip(1.0 + 0.18 * jax.random.normal(splits[4], (D,), jnp.float32), 0.1, 1.9)
    w_query = centred(splits[5], (D, D), D ** -0.5, 0.125, ((1, 16),))
    w_forget = centred(splits[6], (D, D), D ** -0.5, 0.125, ((1, 16),))
    w_input = centred(splits[7], (D, D), D ** -0.5, 0.125, ((1, 16),))
    w_gate = centred(splits[8], (D, D), D ** -0.5, 0.125, ((1, 16),))
    lower_bound = jnp.clip(jax.random.uniform(splits[9], (D,), jnp.float32, 0.05, 0.9), 0.05, 0.9)
    head_gain = jnp.clip(1.0 + 0.18 * jax.random.normal(splits[10], (HEAD_DIM,), jnp.float32), 0.1, 1.9)
    w_out = centred(splits[11], (D, D), D ** -0.5, 0.125, ((1, 16),))
    norm_ffn = jnp.clip(1.0 + 0.18 * jax.random.normal(splits[12], (D,), jnp.float32), 0.1, 1.9)
    expert_gate = centred(splits[13], (D, EXPERTS * FF), D ** -0.5, 0.125, ((1, 16),))
    expert_up = centred(splits[14], (D, EXPERTS * FF), D ** -0.5, 0.125, ((1, 16),))
    expert_down = centred(splits[15], (EXPERTS * FF, D), FF ** -0.5, 0.0625, ((0, 16),))
    return dict(tokens=tokens, state=state, route_ids=route_ids, route_weights=route_weights, norm_mix=norm_mix, w_query=w_query, w_forget=w_forget, w_input=w_input, w_gate=w_gate, lower_bound=lower_bound, head_gain=head_gain, w_out=w_out, norm_ffn=norm_ffn, expert_gate=expert_gate, expert_up=expert_up, expert_down=expert_down)


epsilon = 1e-06

def rms_scale(values, gain):
    return values * lax.rsqrt(lax.optimization_barrier(jnp.mean(values * values, axis=-1, keepdims=True)) + epsilon) * gain

def mixer_state(projected, state, lower_bound, head_gain):
    query_raw = projected[0].astype(jnp.float32)
    forget_raw = projected[1].astype(jnp.float32)
    input_raw = projected[2].astype(jnp.float32)
    gate_raw = projected[3].astype(jnp.float32)
    seq_rows = state.shape[0]
    heads = state.shape[1]
    head_dim = state.shape[2]
    head_shape = (seq_rows, heads, head_dim)
    floor_rate = lower_bound.astype(jnp.float32)
    log_forget = jnp.logaddexp(jnp.log(floor_rate), jnp.log1p(-floor_rate) + jax.nn.log_sigmoid(forget_raw))
    key_vec = (1.0 - floor_rate) * jax.nn.sigmoid(-forget_raw)
    query_vec = jax.nn.silu(query_raw) * head_dim ** (-0.5)
    new_state = jnp.exp(log_forget).reshape(head_shape)[..., None] * state + key_vec.reshape(head_shape)[..., None] * input_raw.reshape(head_shape)[:, :, None, :]
    read_out = jnp.einsum('thk,thkv->thv', query_vec.reshape(head_shape), new_state, precision=lax.Precision.HIGHEST)
    mixed = rms_scale(read_out, head_gain) * jax.nn.silu(gate_raw.reshape(head_shape))
    return (mixed.reshape(seq_rows, heads * head_dim).astype(jnp.bfloat16), new_state)

def reference(tokens, state, route_ids, route_weights, norm_mix, w_query, w_forget, w_input, w_gate, lower_bound, head_gain, w_out, norm_ffn, expert_gate, expert_up, expert_down):
    resid = tokens.astype(jnp.float32)
    normed = rms_scale(resid, norm_mix).astype(jnp.bfloat16)
    projected = jnp.stack([jnp.dot(normed, weight, preferred_element_type=jnp.float32).astype(jnp.bfloat16) for weight in (w_query, w_forget, w_input, w_gate)])
    mixed, new_state = mixer_state(projected, state, lower_bound, head_gain)
    mixer_out = jnp.dot(mixed, w_out, preferred_element_type=jnp.float32).astype(jnp.bfloat16)
    middle = resid + mixer_out.astype(jnp.float32)
    normed_two = rms_scale(middle, norm_ffn).astype(jnp.bfloat16)
    matches = (route_ids[:, :, None] == jnp.arange(EXPERTS, dtype=jnp.int32)[None, None, :]).astype(jnp.float32)
    combined = lax.optimization_barrier(jnp.sum(route_weights.astype(jnp.float32)[:, :, None] * matches, axis=1))
    expert_total = jnp.zeros_like(middle)
    for expert in range(EXPERTS):
        gate_act = jnp.dot(normed_two, expert_gate[:, expert * FF:(expert + 1) * FF], preferred_element_type=jnp.float32)
        up_act = jnp.dot(normed_two, expert_up[:, expert * FF:(expert + 1) * FF], preferred_element_type=jnp.float32)
        hidden = (jax.nn.silu(gate_act) * up_act).astype(jnp.bfloat16)
        down_act = jnp.dot(hidden, expert_down[expert * FF:(expert + 1) * FF, :], preferred_element_type=jnp.float32)
        expert_total = expert_total + combined[:, expert:expert + 1] * down_act
    return ((middle + expert_total).astype(jnp.bfloat16), new_state)
```

```python
import functools

import jax
import jax.numpy as jnp
from jax import lax
from jax.experimental import pallas as pl
from jax.experimental.pallas import tpu as pltpu
from jax.sharding import PartitionSpec as P

FF = 7168
EXPERTS = 4
LANES = 128
MIB = 1 << 20
COST = 10**10

epsilon = 1e-06
f32 = jnp.float32
bf16 = jnp.bfloat16


def call(body, outs, args, name, limit, spaces=None, scratch=(), flops=0, **kwargs):
    spaces = spaces or [pltpu.VMEM] * len(args)
    return pl.pallas_call(
        body,
        out_shape=outs,
        in_specs=[pl.BlockSpec(memory_space=space) for space in spaces],
        out_specs=jax.tree.map(lambda _: pl.BlockSpec(memory_space=pltpu.VMEM), outs),
        scratch_shapes=list(scratch),
        compiler_params=pltpu.CompilerParams(vmem_limit_bytes=limit * MIB),
        cost_estimate=pl.CostEstimate(flops=flops, bytes_accessed=0, transcendentals=0),
        name=name,
        **kwargs,
    )(*args)


def exchange(chunks):
    return lax.all_to_all(chunks, "ep", split_axis=0, concat_axis=0, tiled=True)


def rms(values):
    return values * lax.rsqrt(jnp.mean(values * values, axis=-1, keepdims=True) + epsilon)


def unpack(source, target):
    count, rows = source.shape[0], source.shape[1]
    for i in range(count):
        target[i * rows : (i + 1) * rows, :] = source[i].astype(f32)


def spread_body(rows_ref, out_ref):
    for i in range(out_ref.shape[0]):
        out_ref[i] = rows_ref[...]


def load_body(count, *refs):
    sources, targets, sems = refs[1 : 1 + count], refs[1 + count : 1 + 2 * count], refs[1 + 2 * count]
    copies = [
        pltpu.make_async_copy(source, target, sems.at[i])
        for i, (source, target) in enumerate(zip(sources, targets))
    ]
    for copy in copies:
        copy.start()
    for copy in copies:
        copy.wait()


def load(after, arrays):
    count = len(arrays)
    size = sum(a.size * a.dtype.itemsize for a in arrays)
    return call(
        functools.partial(load_body, count),
        [pltpu.VMEM(a.shape, a.dtype) for a in arrays],
        (after, *arrays),
        "load",
        -(-size // MIB) + 2,
        spaces=[pltpu.VMEM] + [pltpu.HBM] * count,
        scratch=[pltpu.SemaphoreType.DMA((count,))],
        flops=10**9,
    )


def project_body(all_ref, gain_ref, wq_ref, wf_ref, wi_ref, wg_ref, out_ref, rows_ref):
    rows, cols = all_ref.shape[1], wq_ref.shape[1]
    unpack(all_ref, rows_ref)
    normed = (rms(rows_ref[...]) * gain_ref[...]).astype(bf16)
    for p, w_ref in enumerate((wq_ref, wf_ref, wi_ref, wg_ref)):
        product = jnp.dot(normed, w_ref[...], preferred_element_type=f32)
        for i in range(out_ref.shape[0]):
            out_ref[i, :, p * cols : (p + 1) * cols] = product[i * rows : (i + 1) * rows, :].astype(bf16)


def mixer_body(owned_ref, state_ref, bound_ref, gain_ref, out_ref, gates_ref, raw_ref, bounds_ref, read_ref):
    heads, rows = owned_ref.shape[0], owned_ref.shape[1]
    dim = bound_ref.shape[1]
    unpack(owned_ref, raw_ref)
    for h in range(heads):
        bounds_ref[h * rows : (h + 1) * rows, :] = jnp.broadcast_to(bound_ref[h : h + 1, :], (rows, dim))
    bound = bounds_ref[...]
    query_raw, forget_raw, input_raw, gate_raw = (raw_ref[:, p * dim : (p + 1) * dim] for p in range(4))
    decay = bound + (1.0 - bound) * jax.nn.sigmoid(forget_raw)
    key_vec = (1.0 - bound) * jax.nn.sigmoid(-forget_raw)
    query_vec = query_raw * jax.nn.sigmoid(query_raw) * dim ** (-0.5)
    gates_ref[0] = decay
    gates_ref[1] = key_vec
    gates_ref[2] = input_raw
    weights = query_vec * decay
    for start in range(0, heads * rows, 8):
        columns = weights[start : start + 8, :].T
        for p in range(start, min(start + 8, heads * rows)):
            column = columns[:, p - start : p - start + 1]
            read_ref[p : p + 1, :] = jnp.sum(column * state_ref[p % rows, p // rows], axis=0, keepdims=True)
    read = read_ref[...] + jnp.sum(query_vec * key_vec, axis=-1, keepdims=True) * input_raw
    mixed = rms(read) * gain_ref[...] * (gate_raw * jax.nn.sigmoid(gate_raw))
    for h in range(heads):
        block = mixed[h * rows : (h + 1) * rows, :].astype(bf16)
        for i in range(out_ref.shape[0]):
            out_ref[i, :, h * dim : (h + 1) * dim] = block


def update_body(heads_step, gates_ref, state_ref, out_ref, held_ref, in_sem, out_sem):
    rows, heads, dim = state_ref.shape[:3]
    steps = heads // heads_step
    take = rows * heads_step

    def fetch(g):
        part = pl.ds(g * heads_step, heads_step)
        return pltpu.make_async_copy(state_ref.at[:, part], held_ref.at[:, part], in_sem.at[g])

    def put(g):
        part = pl.ds(g * heads_step, heads_step)
        return pltpu.make_async_copy(held_ref.at[:, part], out_ref.at[:, part], out_sem.at[g])

    for g in range(steps):
        fetch(g).start()

    def step(g, carry):
        fetch(g).wait()
        group = pl.ds(g * take, take)
        decay, key_vec = gates_ref[0, group, :].T, gates_ref[1, group, :].T
        value = gates_ref[2, group, :]
        for j in range(take):
            t, h = j % rows, g * heads_step + j // rows
            held_ref[t, h] = decay[:, j : j + 1] * held_ref[t, h] + key_vec[:, j : j + 1] * value[j : j + 1, :]
        put(g).start()
        return carry

    lax.fori_loop(0, steps, step, 0)
    for g in range(steps):
        put(g).wait()


def update(gates, state):
    rows, heads = state.shape[:2]
    heads_step = max(1, 8 // rows)
    steps = heads // heads_step
    return pl.pallas_call(
        functools.partial(update_body, heads_step),
        out_shape=jax.ShapeDtypeStruct(state.shape, f32),
        in_specs=[pl.BlockSpec(memory_space=pltpu.VMEM), pl.BlockSpec(memory_space=pltpu.HBM)],
        out_specs=pl.BlockSpec(memory_space=pltpu.HBM),
        scratch_shapes=[
            pltpu.VMEM(state.shape, f32),
            pltpu.SemaphoreType.DMA((steps,)),
            pltpu.SemaphoreType.DMA((steps,)),
        ],
        compiler_params=pltpu.CompilerParams(vmem_limit_bytes=8 * MIB),
        cost_estimate=pl.CostEstimate(flops=10**9, bytes_accessed=0, transcendentals=0),
        name="update",
    )(gates, state)


def out_body(all_ref, w_ref, out_ref, rows_ref):
    unpack(all_ref, rows_ref)
    product = jnp.dot(rows_ref[...].astype(bf16), w_ref[...], preferred_element_type=f32).astype(bf16)
    for i in range(out_ref.shape[0]):
        out_ref[i] = product


def middle_of(tokens_ref, mixer_ref, target):
    cols = mixer_ref.shape[2]
    unpack(tokens_ref, target)
    for i in range(mixer_ref.shape[0]):
        part = slice(i * cols, (i + 1) * cols)
        target[:, part] = target[:, part] + mixer_ref[i].astype(f32)


def expert_body(tokens_ref, mixer_ref, gain_ref, gate_ref, up_ref, down_ref, out_ref, rows_ref):
    rows = out_ref.shape[1]
    middle_of(tokens_ref, mixer_ref, rows_ref)
    normed = (rms(rows_ref[...]) * gain_ref[...]).astype(bf16)
    gate_act = jnp.dot(normed, gate_ref[...], preferred_element_type=f32)
    up_act = jnp.dot(normed, up_ref[...], preferred_element_type=f32)
    hidden = (gate_act * jax.nn.sigmoid(gate_act) * up_act).astype(bf16)
    product = jnp.dot(hidden, down_ref[...], preferred_element_type=f32)
    for i in range(out_ref.shape[0]):
        out_ref[i] = product[i * rows : (i + 1) * rows, :].astype(bf16)


def own_body(tokens_ref, mixer_ref, out_ref, rows_ref):
    rows = out_ref.shape[0]
    me = lax.axis_index("ep")
    middle_of(tokens_ref, mixer_ref, rows_ref)
    total = jnp.zeros(out_ref.shape, f32)
    for i in range(tokens_ref.shape[0]):
        total = jnp.where(me == i, rows_ref[i * rows : (i + 1) * rows, :], total)
    out_ref[...] = total


def final_body(group, middle_ref, returned_ref, ids_ref, weights_ref, out_ref, shares_ref):
    total = middle_ref[...]
    rows = total.shape[0]
    ids, weights = ids_ref[...], weights_ref[...].astype(f32)
    shares_ref[...] = jnp.zeros(shares_ref.shape, f32)
    for e in range(EXPERTS):
        shares_ref[e : e + 1, :rows] = jnp.sum(jnp.where(ids == e, weights, 0.0), axis=0, keepdims=True)
    shares = shares_ref[...].T
    for e in range(EXPERTS):
        share = shares[:rows, e : e + 1]
        summed = returned_ref[e * group].astype(f32)
        for i in range(e * group + 1, (e + 1) * group):
            summed = summed + returned_ref[i].astype(f32)
        total = total + share * summed
    out_ref[...] = total.astype(bf16)


def local(
    tokens,
    state,
    route_ids,
    route_weights,
    norm_mix,
    w_query,
    w_forget,
    w_input,
    w_gate,
    lower_bound,
    head_gain,
    w_out,
    norm_ffn,
    expert_gate,
    expert_up,
    expert_down,
):
    rows, width = tokens.shape
    heads, dim = state.shape[1], state.shape[2]
    copies = lax.axis_size("ep")
    cols = w_query.shape[1]
    everyone = copies * rows
    group = FF // expert_gate.shape[1]
    shape = jax.ShapeDtypeStruct
    full = shape((copies, rows, width), bf16)

    sent = call(spread_body, full, (tokens,), "spread", 4, flops=COST)
    state_in = state
    all_tokens = exchange(sent)
    projected = call(
        project_body,
        shape((copies, rows, 4 * cols), bf16),
        (all_tokens, norm_mix.reshape(1, width), w_query, w_forget, w_input, w_gate),
        "project",
        8,
        flops=COST,
        scratch=[pltpu.VMEM((everyone, width), f32)],
    )
    owned = exchange(projected)
    if cols != dim:
        owned = owned.reshape(copies, rows, 4, cols).transpose(1, 2, 0, 3).reshape(rows, 4, heads, dim)
        owned = owned.transpose(2, 0, 1, 3).reshape(heads, rows, 4 * dim)
    mixed, gates = call(
        mixer_body,
        [full, shape((3, heads * rows, dim), f32)],
        (owned, state_in, lower_bound.reshape(heads, dim), head_gain.reshape(1, dim)),
        "mixer",
        12,
        flops=COST,
        scratch=[
            pltpu.VMEM((heads * rows, 4 * dim), f32),
            pltpu.VMEM((heads * rows, dim), f32),
            pltpu.VMEM((heads * rows, dim), f32),
        ],
    )
    all_mixed = exchange(mixed)
    mixer_cols = call(
        out_body,
        shape((copies, everyone, cols), bf16),
        (all_mixed, w_out),
        "outward",
        4,
        flops=COST,
        scratch=[pltpu.VMEM((everyone, width), f32)],
    )
    mixer_all = exchange(mixer_cols)
    if cols % LANES:
        mixer_all = mixer_all.transpose(1, 0, 2).reshape(1, everyone, width)
    partials = call(
        expert_body,
        full,
        (all_tokens, mixer_all, norm_ffn.reshape(1, width), expert_gate, expert_up, expert_down),
        "experts",
        30,
        scratch=[pltpu.VMEM((everyone, width), f32)],
    )
    new_state = update(*lax.optimization_barrier((gates, state, partials))[:2])
    returned = exchange(partials)
    middle = call(
        own_body,
        shape((rows, width), f32),
        lax.optimization_barrier((all_tokens, mixer_all, partials))[:2],
        "own",
        4,
        scratch=[pltpu.VMEM((everyone, width), f32)],
        flops=10**8,
    )
    layer_out = call(
        functools.partial(final_body, group),
        shape((rows, width), bf16),
        (middle, returned, route_ids.T, route_weights.T),
        "final",
        4,
        scratch=[pltpu.VMEM((8, LANES), f32)],
    )
    return (layer_out, new_state)


def solution(mesh):
    return jax.shard_map(
        local,
        mesh=mesh,
        in_specs=(
            P(("grp", "ep"), None),
            P(("grp", "ep"), None, None, None),
            P(("grp", "ep"), None),
            P(("grp", "ep"), None),
            P(),
            P(None, "ep"),
            P(None, "ep"),
            P(None, "ep"),
            P(None, "ep"),
            P(),
            P(),
            P(None, "ep"),
            P(),
            P(None, "ep"),
            P(None, "ep"),
            P("ep", None),
        ),
        out_specs=(P(("grp", "ep"), None), P(("grp", "ep"), None, None, None)),
        check_vma=False,
    )
```

```python
import functools

import jax
import jax.numpy as jnp
from jax import lax
from jax.experimental import pallas as pl
from jax.experimental.pallas import tpu as pltpu
from jax.sharding import Mesh
from jax.sharding import PartitionSpec as P

FF = 7168
EXPERTS = 4
LANES = 128
MIB = 1 << 20
COST = 10**10

epsilon = 1e-06
f32 = jnp.float32
bf16 = jnp.bfloat16


def call(body, outs, args, limit, spaces=None, scratch=(), flops=0, **kwargs):
    spaces = spaces or [pltpu.VMEM] * len(args)
    return pl.pallas_call(
        body,
        out_shape=outs,
        in_specs=[pl.BlockSpec(memory_space=space) for space in spaces],
        out_specs=jax.tree.map(lambda _: pl.BlockSpec(memory_space=pltpu.VMEM), outs),
        scratch_shapes=list(scratch),
        compiler_params=pltpu.CompilerParams(vmem_limit_bytes=limit * MIB),
        cost_estimate=pl.CostEstimate(flops=flops, bytes_accessed=0, transcendentals=0),
        **kwargs,
    )(*args)


AXES = ("chip", "core")


def exchange(chunks):
    return lax.all_to_all(chunks, "chip", split_axis=0, concat_axis=0, tiled=True)


def swap(values):
    return lax.ppermute(values, "core", [(0, 1), (1, 0)])


def rms(values):
    return values * lax.rsqrt(jnp.mean(values * values, axis=-1, keepdims=True) + epsilon)


def unpack(source, target):
    count, rows = source.shape[0], source.shape[1]
    for i in range(count):
        target[i * rows : (i + 1) * rows, :] = source[i].astype(f32)


def spread_body(rows_ref, out_ref):
    for i in range(out_ref.shape[0]):
        out_ref[i] = rows_ref[...]


def project_body(all_ref, gain_ref, *refs):
    weights, (out_ref, rows_ref) = refs[:8], refs[8:]
    rows, cols = all_ref.shape[1], weights[0].shape[1]
    core = lax.axis_index("core")
    unpack(all_ref, rows_ref)
    normed = (rms(rows_ref[...]) * gain_ref[...]).astype(bf16)
    for i, w_ref in enumerate(weights):
        p, cross = divmod(i, 2)
        side = 1 - core if cross else core
        product = jnp.dot(normed, w_ref[...], preferred_element_type=f32)
        for chip in range(all_ref.shape[0]):
            block = product[chip * rows : (chip + 1) * rows, :].astype(bf16)
            out_ref[chip, side, :, p * cols : (p + 1) * cols] = block


def mixer_body(owned_ref, state_ref, bound_ref, gain_ref, out_ref, gates_ref, raw_ref, bounds_ref, read_ref):
    heads, rows = owned_ref.shape[0], owned_ref.shape[1]
    dim = bound_ref.shape[1]
    for h in range(heads):
        raw_ref[h * rows : (h + 1) * rows, :] = owned_ref[h].astype(f32)
        bounds_ref[h * rows : (h + 1) * rows, :] = jnp.broadcast_to(bound_ref[h : h + 1, :], (rows, dim))
    bound = bounds_ref[...]
    query_raw, forget_raw, input_raw, gate_raw = (raw_ref[:, p * dim : (p + 1) * dim] for p in range(4))
    decay = bound + (1.0 - bound) * jax.nn.sigmoid(forget_raw)
    key_vec = (1.0 - bound) * jax.nn.sigmoid(-forget_raw)
    query_vec = query_raw * jax.nn.sigmoid(query_raw) * dim ** (-0.5)
    gates_ref[0] = decay
    gates_ref[1] = key_vec
    gates_ref[2] = input_raw
    weights = query_vec * decay
    for start in range(0, heads * rows, 8):
        columns = weights[start : start + 8, :].T
        for p in range(start, min(start + 8, heads * rows)):
            column = columns[:, p - start : p - start + 1]
            read_ref[p : p + 1, :] = jnp.sum(column * state_ref[p % rows, p // rows], axis=0, keepdims=True)
    read = read_ref[...] + jnp.sum(query_vec * key_vec, axis=-1, keepdims=True) * input_raw
    mixed = rms(read) * gain_ref[...] * (gate_raw * jax.nn.sigmoid(gate_raw))
    for h in range(heads):
        block = mixed[h * rows : (h + 1) * rows, :].astype(bf16)
        for i in range(out_ref.shape[0]):
            out_ref[i, :, h * dim : (h + 1) * dim] = block


def out_body(all_ref, own_ref, cross_ref, out_ref, rows_ref):
    core = lax.axis_index("core")
    unpack(all_ref, rows_ref)
    mixed = rows_ref[...].astype(bf16)
    for side, w_ref in ((core, own_ref), (1 - core, cross_ref)):
        block = jnp.dot(mixed, w_ref[...], preferred_element_type=f32).astype(bf16)
        for i in range(out_ref.shape[0]):
            out_ref[i, side] = block


def norm_body(tokens_ref, mixer_ref, gain_ref, normed_ref, middle_ref, rows_ref):
    rows, cols = middle_ref.shape[1], mixer_ref.shape[3]
    unpack(tokens_ref, rows_ref)
    for chip in range(mixer_ref.shape[0]):
        for side in range(2):
            part = slice((2 * chip + side) * cols, (2 * chip + side + 1) * cols)
            rows_ref[:, part] = rows_ref[:, part] + mixer_ref[chip, side].astype(f32)
    normed_ref[...] = (rms(rows_ref[...]) * gain_ref[...]).astype(bf16)
    for chip in range(middle_ref.shape[0]):
        middle_ref[chip] = rows_ref[chip * rows : (chip + 1) * rows, :]


def expert_body(
    mine_ref,
    other_ref,
    gate_ref,
    up_ref,
    down_ref,
    gates_ref,
    state_ref,
    keep_ref,
    send_ref,
    new_ref,
    normed_ref,
    hidden_ref,
    held_ref,
    sems,
):
    chips, rows = keep_ref.shape[:2]
    half = mine_ref.shape[0]
    hidden_cols, width = gate_ref.shape[1], down_ref.shape[1]
    seqs, heads = state_ref.shape[:2]
    step = 2 * LANES
    blocks = [pl.ds(i, min(step, hidden_cols - i)) for i in range(0, hidden_cols, step)]
    parts = [pl.ds(i, min(step, width - i)) for i in range(0, width, step)]
    normed_ref[:half, :] = mine_ref[...]
    normed_ref[half:, :] = other_ref[...]
    normed = normed_ref[...]
    copies = []

    def renew(h):
        group = slice(h * seqs, (h + 1) * seqs)
        decay, key_vec, value = gates_ref[0, group, :].T, gates_ref[1, group, :].T, gates_ref[2, group, :]
        for t in range(seqs):
            held_ref[t, h] = decay[:, t : t + 1] * state_ref[t, h] + key_vec[:, t : t + 1] * value[t : t + 1, :]
        copies.append(pltpu.make_async_copy(held_ref.at[:, h], new_ref.at[:, h], sems.at[h]))
        copies[-1].start()

    for i, block in enumerate(blocks):
        gate_act = jnp.dot(normed, gate_ref[:, block], preferred_element_type=f32)
        up_act = jnp.dot(normed, up_ref[:, block], preferred_element_type=f32)
        for h in range(i * heads // len(blocks), (i + 1) * heads // len(blocks)):
            renew(h)
        hidden_ref[:, block] = (gate_act * jax.nn.sigmoid(gate_act) * up_act).astype(bf16)
    hidden = hidden_ref[...]
    for part in parts:
        product = jnp.dot(hidden, down_ref[:, part], preferred_element_type=f32)
        for side, out_ref in enumerate((keep_ref, send_ref)):
            for chip in range(chips):
                start = (side * chips + chip) * rows
                out_ref[chip, :, part] = product[start : start + rows, :].astype(out_ref.dtype)
    for copy in copies:
        copy.wait()


def add_body(keep_ref, came_ref, out_ref):
    out_ref[...] = (keep_ref[...] + came_ref[...].astype(f32)).astype(bf16)


def final_body(group, middle_ref, returned_ref, ids_ref, weights_ref, out_ref, shares_ref):
    total = middle_ref[lax.axis_index("chip")]
    rows = total.shape[0]
    ids, weights = ids_ref[...], weights_ref[...].astype(f32)
    shares_ref[...] = jnp.zeros(shares_ref.shape, f32)
    for e in range(EXPERTS):
        shares_ref[e : e + 1, :rows] = jnp.sum(jnp.where(ids == e, weights, 0.0), axis=0, keepdims=True)
    shares = shares_ref[...].T
    for e in range(EXPERTS):
        share = shares[:rows, e : e + 1]
        summed = returned_ref[e * group].astype(f32)
        for i in range(e * group + 1, (e + 1) * group):
            summed = summed + returned_ref[i].astype(f32)
        total = total + share * summed
    out_ref[...] = total.astype(bf16)


def body(
    tokens,
    state,
    route_ids,
    route_weights,
    norm_mix,
    w_query,
    w_forget,
    w_input,
    w_gate,
    lower_bound,
    head_gain,
    w_out,
    norm_ffn,
    expert_gate,
    expert_up,
    expert_down,
):
    rows, width = tokens.shape
    heads, dim = state.shape[1], state.shape[2]
    chips = lax.axis_size("chip")
    cols = w_query.shape[1]
    half = chips * rows
    group = FF // expert_gate.shape[1] // 2
    shape = jax.ShapeDtypeStruct
    full = shape((chips, rows, width), bf16)
    rows_scratch = [pltpu.VMEM((half, width), f32)]

    weights = []
    for weight in (w_query, w_forget, w_input, w_gate, w_out):
        weights += [weight, swap(weight)]
    sent = call(spread_body, full, (tokens,), 4, flops=COST)
    all_tokens = exchange(sent)
    all_tokens, out_cross = lax.optimization_barrier((all_tokens, weights[9]))
    projected = call(
        project_body,
        shape((chips, 2, rows, 4 * cols), bf16),
        (all_tokens, norm_mix.reshape(1, width), *weights[:8]),
        8,
        scratch=rows_scratch,
        flops=COST,
    )
    owned = exchange(projected).reshape(2 * chips, rows, 4 * cols)
    if cols != dim:
        owned = owned.reshape(2 * chips, rows, 4, cols).transpose(1, 2, 0, 3).reshape(rows, 4, heads, dim)
        owned = owned.transpose(2, 0, 1, 3).reshape(heads, rows, 4 * dim)
    mixed, gates = call(
        mixer_body,
        [full, shape((3, heads * rows, dim), f32)],
        (owned, state, lower_bound.reshape(heads, dim), head_gain.reshape(1, dim)),
        12,
        flops=COST,
        scratch=[
            pltpu.VMEM((heads * rows, 4 * dim), f32),
            pltpu.VMEM((heads * rows, dim), f32),
            pltpu.VMEM((heads * rows, dim), f32),
        ],
    )
    mixer_cols = call(
        out_body,
        shape((chips, 2, half, cols), bf16),
        (exchange(mixed), w_out, out_cross),
        6,
        flops=COST,
        scratch=rows_scratch,
    )
    normed, middle = call(
        norm_body,
        [shape((half, width), bf16), shape((chips, rows, width), f32)],
        (all_tokens, exchange(mixer_cols), norm_ffn.reshape(1, width)),
        6,
        flops=COST,
        scratch=rows_scratch,
    )
    vmem = pl.BlockSpec(memory_space=pltpu.VMEM)
    keep, send, new_state = pl.pallas_call(
        expert_body,
        out_shape=[shape((chips, rows, width), f32), full, shape(state.shape, f32)],
        in_specs=[vmem] * 7,
        out_specs=[vmem, vmem, pl.BlockSpec(memory_space=pltpu.HBM)],
        scratch_shapes=[
            pltpu.VMEM((2 * half, width), bf16),
            pltpu.VMEM((2 * half, expert_gate.shape[1]), bf16),
            pltpu.VMEM(state.shape, f32),
            pltpu.SemaphoreType.DMA((heads,)),
        ],
        compiler_params=pltpu.CompilerParams(vmem_limit_bytes=14 * MIB),
        cost_estimate=pl.CostEstimate(flops=COST, bytes_accessed=0, transcendentals=0),
        name="experts",
    )(normed, swap(normed), expert_gate, expert_up, expert_down, gates, state)
    partials = call(add_body, full, (keep, swap(send)), 4)
    returned = exchange(partials)
    layer_out = call(
        functools.partial(final_body, group),
        shape((rows, width), bf16),
        (middle, returned, route_ids.T, route_weights.T),
        4,
        scratch=[pltpu.VMEM((8, LANES), f32)],
    )
    return (layer_out, new_state)


def solution(mesh):
    groups, size = mesh.shape["grp"], mesh.shape["ep"]
    split = Mesh(mesh.devices.reshape(groups, size // 2, 2), ("grp", *AXES))
    return jax.shard_map(
        body,
        mesh=split,
        in_specs=(
            P(("grp", *AXES), None),
            P(("grp", *AXES), None, None, None),
            P(("grp", *AXES), None),
            P(("grp", *AXES), None),
            P(),
            P(None, AXES),
            P(None, AXES),
            P(None, AXES),
            P(None, AXES),
            P(),
            P(),
            P(None, AXES),
            P(),
            P(None, AXES),
            P(None, AXES),
            P(AXES, None),
        ),
        out_specs=(P(("grp", *AXES), None), P(("grp", *AXES), None, None, None)),
        check_vma=False,
    )
```

```python
import functools

import jax
import jax.numpy as jnp
from jax import lax
from jax.experimental import pallas as pl
from jax.experimental.pallas import tpu as pltpu
from jax.sharding import Mesh
from jax.sharding import PartitionSpec as P

FF = 7168
EXPERTS = 4
LANES = 128
MIB = 1 << 20
COST = 10**10

epsilon = 1e-06
f32 = jnp.float32
bf16 = jnp.bfloat16


def call(body, outs, args, limit, spaces=None, scratch=(), flops=0, **kwargs):
    spaces = spaces or [pltpu.VMEM] * len(args)
    return pl.pallas_call(
        body,
        out_shape=outs,
        in_specs=[pl.BlockSpec(memory_space=space) for space in spaces],
        out_specs=jax.tree.map(lambda _: pl.BlockSpec(memory_space=pltpu.VMEM), outs),
        scratch_shapes=list(scratch),
        compiler_params=pltpu.CompilerParams(vmem_limit_bytes=limit * MIB),
        cost_estimate=pl.CostEstimate(flops=flops, bytes_accessed=0, transcendentals=0),
        **kwargs,
    )(*args)


AXES = ("chip", "core")


def exchange(chunks):
    return lax.all_to_all(chunks, "chip", split_axis=0, concat_axis=0, tiled=True)


def swap(values):
    return lax.ppermute(values, "core", [(0, 1), (1, 0)])


def rms(values):
    return values * lax.rsqrt(jnp.mean(values * values, axis=-1, keepdims=True) + epsilon)


def unpack(source, target):
    count, rows = source.shape[0], source.shape[1]
    for i in range(count):
        target[i * rows : (i + 1) * rows, :] = source[i].astype(f32)


def mark_body(out_ref):
    out_ref[...] = jnp.zeros(out_ref.shape, out_ref.dtype)


def spread_body(rows_ref, mark_ref, out_ref):
    for i in range(out_ref.shape[0]):
        out_ref[i] = rows_ref[...]


def project_body(all_ref, gain_ref, *refs):
    weights, (out_ref, rows_ref) = refs[:8], refs[8:]
    rows, cols = all_ref.shape[1], weights[0].shape[1]
    core = lax.axis_index("core")
    unpack(all_ref, rows_ref)
    normed = (rms(rows_ref[...]) * gain_ref[...]).astype(bf16)
    for i, w_ref in enumerate(weights):
        p, cross = divmod(i, 2)
        side = 1 - core if cross else core
        product = jnp.dot(normed, w_ref[...], preferred_element_type=f32)
        for chip in range(all_ref.shape[0]):
            block = product[chip * rows : (chip + 1) * rows, :].astype(bf16)
            out_ref[chip, side, :, p * cols : (p + 1) * cols] = block


def thirds(values):
    first = values.astype(bf16).astype(f32)
    second = (values - first).astype(bf16).astype(f32)
    return first, second, (values - first - second).astype(bf16).astype(f32)


def chooser(count, dim):
    shape = (3 * count, count * dim)
    row, column = lax.broadcasted_iota(jnp.int32, shape, 0), lax.broadcasted_iota(jnp.int32, shape, 1)
    return (row % count == column // dim).astype(f32)


def mixer_body(owned_ref, state_ref, bound_ref, gain_ref, out_ref, gates_ref, raw_ref, bounds_ref, read_ref):
    heads, rows = owned_ref.shape[0], owned_ref.shape[1]
    dim = bound_ref.shape[1]
    for h in range(heads):
        raw_ref[h * rows : (h + 1) * rows, :] = owned_ref[h].astype(f32)
        bounds_ref[h * rows : (h + 1) * rows, :] = jnp.broadcast_to(bound_ref[h : h + 1, :], (rows, dim))
    bound = bounds_ref[...]
    query_raw, forget_raw, input_raw, gate_raw = (raw_ref[:, p * dim : (p + 1) * dim] for p in range(4))
    decay = bound + (1.0 - bound) * jax.nn.sigmoid(forget_raw)
    key_vec = (1.0 - bound) * jax.nn.sigmoid(-forget_raw)
    query_vec = query_raw * jax.nn.sigmoid(query_raw) * dim ** (-0.5)
    gates_ref[0] = decay
    gates_ref[1] = key_vec
    gates_ref[2] = input_raw
    weights = thirds(query_vec * decay)
    take = min(16, heads * rows)
    chosen = chooser(take, dim).astype(bf16)
    for start in range(0, heads * rows, take):
        columns = jnp.concatenate([part[start : start + take, :] for part in weights], axis=0).T
        wide = jnp.dot(columns.astype(bf16), chosen, preferred_element_type=f32)
        for j in range(take):
            h, t = divmod(start + j, rows)
            product = wide[:, j * dim : (j + 1) * dim] * state_ref[t, h]
            read_ref[start + j : start + j + 1, :] = jnp.sum(product, axis=0, keepdims=True)
    read = read_ref[...] + jnp.sum(query_vec * key_vec, axis=-1, keepdims=True) * input_raw
    mixed = rms(read) * gain_ref[...] * (gate_raw * jax.nn.sigmoid(gate_raw))
    for h in range(heads):
        block = mixed[h * rows : (h + 1) * rows, :].astype(bf16)
        for i in range(out_ref.shape[0]):
            out_ref[i, :, h * dim : (h + 1) * dim] = block


def out_body(all_ref, own_ref, cross_ref, out_ref, rows_ref):
    core = lax.axis_index("core")
    unpack(all_ref, rows_ref)
    mixed = rows_ref[...].astype(bf16)
    for side, w_ref in ((core, own_ref), (1 - core, cross_ref)):
        block = jnp.dot(mixed, w_ref[...], preferred_element_type=f32).astype(bf16)
        for i in range(out_ref.shape[0]):
            out_ref[i, side] = block


def norm_body(tokens_ref, mixer_ref, gain_ref, normed_ref, middle_ref, rows_ref):
    rows, cols = middle_ref.shape[1], mixer_ref.shape[3]
    unpack(tokens_ref, rows_ref)
    for chip in range(mixer_ref.shape[0]):
        for side in range(2):
            part = slice((2 * chip + side) * cols, (2 * chip + side + 1) * cols)
            rows_ref[:, part] = rows_ref[:, part] + mixer_ref[chip, side].astype(f32)
    normed_ref[...] = (rms(rows_ref[...]) * gain_ref[...]).astype(bf16)
    for chip in range(middle_ref.shape[0]):
        middle_ref[chip] = rows_ref[chip * rows : (chip + 1) * rows, :]


def expert_body(
    mine_ref,
    other_ref,
    gate_ref,
    up_ref,
    down_ref,
    gates_ref,
    state_ref,
    keep_ref,
    send_ref,
    new_ref,
    normed_ref,
    hidden_ref,
    held_ref,
    sems,
):
    chips, rows = keep_ref.shape[:2]
    half = mine_ref.shape[0]
    hidden_cols, width = gate_ref.shape[1], down_ref.shape[1]
    seqs, heads, dim = state_ref.shape[:3]
    step_heads = max(1, 8 // seqs)
    take, groups = step_heads * seqs, heads // step_heads
    step = 2 * LANES
    blocks = [pl.ds(i, min(step, hidden_cols - i)) for i in range(0, hidden_cols, step)]
    parts = [pl.ds(i, min(step, width - i)) for i in range(0, width, step)]
    normed_ref[:half, :] = mine_ref[...]
    normed_ref[half:, :] = other_ref[...]
    normed = normed_ref[...]
    copies = []

    chosen = chooser(take, dim)

    def renew(g):
        group = slice(g * take, (g + 1) * take)
        decay, key_vec, value = gates_ref[0, group, :].T, thirds(gates_ref[1, group, :]), gates_ref[2, group, :]
        columns = jnp.concatenate(key_vec, axis=0).T.astype(bf16)
        values = jnp.concatenate([jnp.concatenate([value] * 3, axis=0)] * take, axis=1) * chosen
        outer = jnp.dot(columns, values.astype(bf16), preferred_element_type=f32)
        for j in range(take):
            h, t = divmod(g * take + j, seqs)
            held_ref[t, h] = decay[:, j : j + 1] * state_ref[t, h] + outer[:, j * dim : (j + 1) * dim]
        part = pl.ds(g * step_heads, step_heads)
        copies.append(pltpu.make_async_copy(held_ref.at[:, part], new_ref.at[:, part], sems.at[g]))
        copies[-1].start()

    for i, block in enumerate(blocks):
        gate_act = jnp.dot(normed, gate_ref[:, block], preferred_element_type=f32)
        up_act = jnp.dot(normed, up_ref[:, block], preferred_element_type=f32)
        for g in range(i * groups // len(blocks), (i + 1) * groups // len(blocks)):
            renew(g)
        hidden_ref[:, block] = (gate_act * jax.nn.sigmoid(gate_act) * up_act).astype(bf16)
    hidden = hidden_ref[...]
    for part in parts:
        product = jnp.dot(hidden, down_ref[:, part], preferred_element_type=f32)
        for side, out_ref in enumerate((keep_ref, send_ref)):
            for chip in range(chips):
                start = (side * chips + chip) * rows
                out_ref[chip, :, part] = product[start : start + rows, :].astype(out_ref.dtype)
    for copy in copies:
        copy.wait()


def add_body(keep_ref, came_ref, out_ref):
    out_ref[...] = (keep_ref[...] + came_ref[...].astype(f32)).astype(bf16)


def final_body(group, middle_ref, returned_ref, ids_ref, weights_ref, out_ref, shares_ref):
    total = middle_ref[lax.axis_index("chip")]
    rows = total.shape[0]
    ids, weights = ids_ref[...], weights_ref[...].astype(f32)
    shares_ref[...] = jnp.zeros(shares_ref.shape, f32)
    for e in range(EXPERTS):
        shares_ref[e : e + 1, :rows] = jnp.sum(jnp.where(ids == e, weights, 0.0), axis=0, keepdims=True)
    shares = shares_ref[...].T
    for e in range(EXPERTS):
        share = shares[:rows, e : e + 1]
        summed = returned_ref[e * group].astype(f32)
        for i in range(e * group + 1, (e + 1) * group):
            summed = summed + returned_ref[i].astype(f32)
        total = total + share * summed
    out_ref[...] = total.astype(bf16)


def body(
    tokens,
    state,
    route_ids,
    route_weights,
    norm_mix,
    w_query,
    w_forget,
    w_input,
    w_gate,
    lower_bound,
    head_gain,
    w_out,
    norm_ffn,
    expert_gate,
    expert_up,
    expert_down,
):
    rows, width = tokens.shape
    heads, dim = state.shape[1], state.shape[2]
    chips = lax.axis_size("chip")
    cols = w_query.shape[1]
    half = chips * rows
    group = FF // expert_gate.shape[1] // 2
    shape = jax.ShapeDtypeStruct
    full = shape((chips, rows, width), bf16)
    rows_scratch = [pltpu.VMEM((half, width), f32)]

    weights = []
    for weight in (w_query, w_forget, w_input, w_gate, w_out):
        weights += [weight, swap(weight)]
    mark = call(mark_body, shape((8, LANES), f32), (), 1, flops=COST)
    sent = call(spread_body, full, (tokens, mark), 4, flops=COST)
    all_tokens = exchange(sent)
    all_tokens, out_cross = lax.optimization_barrier((all_tokens, weights[9]))
    projected = call(
        project_body,
        shape((chips, 2, rows, 4 * cols), bf16),
        (all_tokens, norm_mix.reshape(1, width), *weights[:8]),
        8,
        scratch=rows_scratch,
    )
    owned = exchange(projected).reshape(2 * chips, rows, 4 * cols)
    if cols != dim:
        owned = owned.reshape(2 * chips, rows, 4, cols).transpose(1, 2, 0, 3).reshape(rows, 4, heads, dim)
        owned = owned.transpose(2, 0, 1, 3).reshape(heads, rows, 4 * dim)
    mixed, gates = call(
        mixer_body,
        [full, shape((3, heads * rows, dim), f32)],
        (owned, state, lower_bound.reshape(heads, dim), head_gain.reshape(1, dim)),
        12,
        scratch=[
            pltpu.VMEM((heads * rows, 4 * dim), f32),
            pltpu.VMEM((heads * rows, dim), f32),
            pltpu.VMEM((heads * rows, dim), f32),
        ],
    )
    mixer_cols = call(
        out_body, shape((chips, 2, half, cols), bf16), (exchange(mixed), w_out, out_cross), 6, scratch=rows_scratch
    )
    normed, middle = call(
        norm_body,
        [shape((half, width), bf16), shape((chips, rows, width), f32)],
        (all_tokens, exchange(mixer_cols), norm_ffn.reshape(1, width)),
        6,
        scratch=rows_scratch,
    )
    vmem = pl.BlockSpec(memory_space=pltpu.VMEM)
    keep, send, new_state = pl.pallas_call(
        expert_body,
        out_shape=[shape((chips, rows, width), f32), full, shape(state.shape, f32)],
        in_specs=[vmem] * 7,
        out_specs=[vmem, vmem, pl.BlockSpec(memory_space=pltpu.HBM)],
        scratch_shapes=[
            pltpu.VMEM((2 * half, width), bf16),
            pltpu.VMEM((2 * half, expert_gate.shape[1]), bf16),
            pltpu.VMEM(state.shape, f32),
            pltpu.SemaphoreType.DMA((heads,)),
        ],
        compiler_params=pltpu.CompilerParams(vmem_limit_bytes=14 * MIB),
        cost_estimate=pl.CostEstimate(flops=COST, bytes_accessed=0, transcendentals=0),
        name="experts",
    )(normed, swap(normed), expert_gate, expert_up, expert_down, gates, state)
    partials = call(add_body, full, (keep, swap(send)), 4)
    returned = exchange(partials)
    layer_out = call(
        functools.partial(final_body, group),
        shape((rows, width), bf16),
        (middle, returned, route_ids.T, route_weights.T),
        4,
        scratch=[pltpu.VMEM((8, LANES), f32)],
    )
    return (layer_out, new_state)


def solution(mesh):
    groups, size = mesh.shape["grp"], mesh.shape["ep"]
    split = Mesh(mesh.devices.reshape(groups, size // 2, 2), ("grp", *AXES))
    return jax.shard_map(
        body,
        mesh=split,
        in_specs=(
            P(("grp", *AXES), None),
            P(("grp", *AXES), None, None, None),
            P(("grp", *AXES), None),
            P(("grp", *AXES), None),
            P(),
            P(None, AXES),
            P(None, AXES),
            P(None, AXES),
            P(None, AXES),
            P(),
            P(),
            P(None, AXES),
            P(),
            P(None, AXES),
            P(None, AXES),
            P(AXES, None),
        ),
        out_specs=(P(("grp", *AXES), None), P(("grp", *AXES), None, None, None)),
        check_vma=False,
    )
```

```python
import functools

import jax
import jax.numpy as jnp
from jax import lax
from jax.experimental import pallas as pl
from jax.experimental.pallas import tpu as pltpu
from jax.sharding import Mesh
from jax.sharding import PartitionSpec as P

FF = 7168
EXPERTS = 4
LANES = 128
MIB = 1 << 20
COST = 10**10

epsilon = 1e-06
f32 = jnp.float32
bf16 = jnp.bfloat16


def call(body, outs, args, limit, spaces=None, scratch=(), flops=0, **kwargs):
    spaces = spaces or [pltpu.VMEM] * len(args)
    return pl.pallas_call(
        body,
        out_shape=outs,
        in_specs=[pl.BlockSpec(memory_space=space) for space in spaces],
        out_specs=jax.tree.map(lambda _: pl.BlockSpec(memory_space=pltpu.VMEM), outs),
        scratch_shapes=list(scratch),
        compiler_params=pltpu.CompilerParams(vmem_limit_bytes=limit * MIB),
        cost_estimate=pl.CostEstimate(flops=flops, bytes_accessed=0, transcendentals=0),
        **kwargs,
    )(*args)


AXES = ("chip", "core")


def chip_order():
    half = lax.axis_size("chip") // 2
    inward = [i // 2 if i % 2 == 0 else half - 1 - i // 2 for i in range(half)]
    return [2 * i + odd for odd in range(2) for i in inward]


def my_place():
    chip, half = lax.axis_index("chip"), lax.axis_size("chip") // 2
    i = chip // 2
    return (chip % 2) * half + jnp.where(2 * i < half, 2 * i, 2 * (half - 1 - i) + 1)


def lines():
    return [[2 * chip + (line ^ chip % 2) for chip in chip_order()] for line in range(2)]


def exchange(chunks):
    return lax.all_to_all(chunks, AXES, split_axis=0, concat_axis=0, axis_index_groups=lines(), tiled=True)


def swap(values):
    return lax.ppermute(values, "core", [(0, 1), (1, 0)])


def rms(values):
    return values * lax.rsqrt(jnp.mean(values * values, axis=-1, keepdims=True) + epsilon)


def unpack(source, target):
    count, rows = source.shape[0], source.shape[1]
    for i in range(count):
        target[i * rows : (i + 1) * rows, :] = source[i].astype(f32)


def mark_body(out_ref):
    out_ref[...] = jnp.zeros(out_ref.shape, out_ref.dtype)


def spread_body(rows_ref, mark_ref, out_ref):
    for i in range(out_ref.shape[0]):
        out_ref[i] = rows_ref[...]


def project_body(all_ref, gain_ref, *refs):
    weights, (out_ref, rows_ref) = refs[:8], refs[8:]
    rows, cols = all_ref.shape[1], weights[0].shape[1]
    core = lax.axis_index("core")
    unpack(all_ref, rows_ref)
    normed = (rms(rows_ref[...]) * gain_ref[...]).astype(bf16)
    for i, w_ref in enumerate(weights):
        p, cross = divmod(i, 2)
        side = 1 - core if cross else core
        product = jnp.dot(normed, w_ref[...], preferred_element_type=f32)
        for chip in range(all_ref.shape[0]):
            block = product[chip * rows : (chip + 1) * rows, :].astype(bf16)
            out_ref[chip, side, :, p * cols : (p + 1) * cols] = block


def thirds(values):
    first = values.astype(bf16).astype(f32)
    second = (values - first).astype(bf16).astype(f32)
    return first, second, (values - first - second).astype(bf16).astype(f32)


def chooser(count, dim):
    shape = (3 * count, count * dim)
    row, column = lax.broadcasted_iota(jnp.int32, shape, 0), lax.broadcasted_iota(jnp.int32, shape, 1)
    return (row % count == column // dim).astype(f32)


def mixer_body(source, owned_ref, state_ref, bound_ref, gain_ref, out_ref, gates_ref, raw_ref, bounds_ref, read_ref):
    heads, rows = owned_ref.shape[0], owned_ref.shape[1]
    dim = bound_ref.shape[1]
    for h in range(heads):
        raw_ref[h * rows : (h + 1) * rows, :] = owned_ref[source[h]].astype(f32)
        bounds_ref[h * rows : (h + 1) * rows, :] = jnp.broadcast_to(bound_ref[h : h + 1, :], (rows, dim))
    bound = bounds_ref[...]
    query_raw, forget_raw, input_raw, gate_raw = (raw_ref[:, p * dim : (p + 1) * dim] for p in range(4))
    decay = bound + (1.0 - bound) * jax.nn.sigmoid(forget_raw)
    key_vec = (1.0 - bound) * jax.nn.sigmoid(-forget_raw)
    query_vec = query_raw * jax.nn.sigmoid(query_raw) * dim ** (-0.5)
    gates_ref[0] = decay
    gates_ref[1] = key_vec
    gates_ref[2] = input_raw
    weights = thirds(query_vec * decay)
    take = min(16, heads * rows)
    chosen = chooser(take, dim).astype(bf16)
    for start in range(0, heads * rows, take):
        columns = jnp.concatenate([part[start : start + take, :] for part in weights], axis=0).T
        wide = jnp.dot(columns.astype(bf16), chosen, preferred_element_type=f32)
        for j in range(take):
            h, t = divmod(start + j, rows)
            product = wide[:, j * dim : (j + 1) * dim] * state_ref[t, h]
            read_ref[start + j : start + j + 1, :] = jnp.sum(product, axis=0, keepdims=True)
    read = read_ref[...] + jnp.sum(query_vec * key_vec, axis=-1, keepdims=True) * input_raw
    mixed = rms(read) * gain_ref[...] * (gate_raw * jax.nn.sigmoid(gate_raw))
    for h in range(heads):
        block = mixed[h * rows : (h + 1) * rows, :].astype(bf16)
        for i in range(out_ref.shape[0]):
            out_ref[i, :, h * dim : (h + 1) * dim] = block


def out_body(all_ref, own_ref, cross_ref, out_ref, rows_ref):
    core = lax.axis_index("core")
    unpack(all_ref, rows_ref)
    mixed = rows_ref[...].astype(bf16)
    for side, w_ref in ((core, own_ref), (1 - core, cross_ref)):
        block = jnp.dot(mixed, w_ref[...], preferred_element_type=f32).astype(bf16)
        for i in range(out_ref.shape[0]):
            out_ref[i, side] = block


def norm_body(tokens_ref, mixer_ref, gain_ref, normed_ref, middle_ref, rows_ref):
    rows, cols = middle_ref.shape[1], mixer_ref.shape[3]
    unpack(tokens_ref, rows_ref)
    for place, chip in enumerate(chip_order()):
        for side in range(2):
            part = slice((2 * chip + side) * cols, (2 * chip + side + 1) * cols)
            rows_ref[:, part] = rows_ref[:, part] + mixer_ref[place, side].astype(f32)
    normed_ref[...] = (rms(rows_ref[...]) * gain_ref[...]).astype(bf16)
    for chip in range(middle_ref.shape[0]):
        middle_ref[chip] = rows_ref[chip * rows : (chip + 1) * rows, :]


def expert_body(
    mine_ref,
    other_ref,
    gate_ref,
    up_ref,
    down_ref,
    gates_ref,
    state_ref,
    keep_ref,
    send_ref,
    new_ref,
    normed_ref,
    hidden_ref,
    held_ref,
    sems,
):
    chips, rows = keep_ref.shape[:2]
    half = mine_ref.shape[0]
    hidden_cols, width = gate_ref.shape[1], down_ref.shape[1]
    seqs, heads, dim = state_ref.shape[:3]
    step_heads = max(1, 8 // seqs)
    take, groups = step_heads * seqs, heads // step_heads
    step = 2 * LANES
    blocks = [pl.ds(i, min(step, hidden_cols - i)) for i in range(0, hidden_cols, step)]
    parts = [pl.ds(i, min(step, width - i)) for i in range(0, width, step)]
    normed_ref[:half, :] = mine_ref[...]
    normed_ref[half:, :] = other_ref[...]
    normed = normed_ref[...]
    copies = []

    chosen = chooser(take, dim)

    def renew(g):
        group = slice(g * take, (g + 1) * take)
        decay, key_vec, value = gates_ref[0, group, :].T, thirds(gates_ref[1, group, :]), gates_ref[2, group, :]
        columns = jnp.concatenate(key_vec, axis=0).T.astype(bf16)
        values = jnp.concatenate([jnp.concatenate([value] * 3, axis=0)] * take, axis=1) * chosen
        outer = jnp.dot(columns, values.astype(bf16), preferred_element_type=f32)
        for j in range(take):
            h, t = divmod(g * take + j, seqs)
            held_ref[t, h] = decay[:, j : j + 1] * state_ref[t, h] + outer[:, j * dim : (j + 1) * dim]
        part = pl.ds(g * step_heads, step_heads)
        copies.append(pltpu.make_async_copy(held_ref.at[:, part], new_ref.at[:, part], sems.at[g]))
        copies[-1].start()

    for i, block in enumerate(blocks):
        gate_act = jnp.dot(normed, gate_ref[:, block], preferred_element_type=f32)
        up_act = jnp.dot(normed, up_ref[:, block], preferred_element_type=f32)
        for g in range(i * groups // len(blocks), (i + 1) * groups // len(blocks)):
            renew(g)
        hidden_ref[:, block] = (gate_act * jax.nn.sigmoid(gate_act) * up_act).astype(bf16)
    hidden = hidden_ref[...]
    for part in parts:
        product = jnp.dot(hidden, down_ref[:, part], preferred_element_type=f32)
        for side, out_ref in enumerate((keep_ref, send_ref)):
            for chip in range(chips):
                start = (side * chips + chip) * rows
                out_ref[chip, :, part] = product[start : start + rows, :].astype(out_ref.dtype)
    for copy in copies:
        copy.wait()


def add_body(keep_ref, came_ref, out_ref):
    out_ref[...] = (keep_ref[...] + came_ref[...].astype(f32)).astype(bf16)


def final_body(group, middle_ref, returned_ref, ids_ref, weights_ref, out_ref, shares_ref):
    total = middle_ref[my_place()]
    rows = total.shape[0]
    ids, weights = ids_ref[...], weights_ref[...].astype(f32)
    shares_ref[...] = jnp.zeros(shares_ref.shape, f32)
    for e in range(EXPERTS):
        shares_ref[e : e + 1, :rows] = jnp.sum(jnp.where(ids == e, weights, 0.0), axis=0, keepdims=True)
    shares = shares_ref[...].T
    for e in range(EXPERTS):
        share = shares[:rows, e : e + 1]
        places = [place for place, chip in enumerate(chip_order()) if chip // group == e]
        summed = returned_ref[places[0]].astype(f32)
        for place in places[1:]:
            summed = summed + returned_ref[place].astype(f32)
        total = total + share * summed
    out_ref[...] = total.astype(bf16)


def body(
    tokens,
    state,
    route_ids,
    route_weights,
    norm_mix,
    w_query,
    w_forget,
    w_input,
    w_gate,
    lower_bound,
    head_gain,
    w_out,
    norm_ffn,
    expert_gate,
    expert_up,
    expert_down,
):
    rows, width = tokens.shape
    heads, dim = state.shape[1], state.shape[2]
    chips = lax.axis_size("chip")
    cols = w_query.shape[1]
    half = chips * rows
    group = FF // expert_gate.shape[1] // 2
    shape = jax.ShapeDtypeStruct
    full = shape((chips, rows, width), bf16)
    rows_scratch = [pltpu.VMEM((half, width), f32)]

    weights = []
    for weight in (w_query, w_forget, w_input, w_gate, w_out):
        weights += [weight, swap(weight)]
    mark = call(mark_body, shape((8, LANES), f32), (), 1, flops=COST)
    sent = call(spread_body, full, (tokens, mark), 4, flops=COST)
    all_tokens = exchange(sent)
    all_tokens, out_cross = lax.optimization_barrier((all_tokens, weights[9]))
    projected = call(
        project_body,
        shape((chips, 2, rows, 4 * cols), bf16),
        (all_tokens, norm_mix.reshape(1, width), *weights[:8]),
        8,
        scratch=rows_scratch,
    )
    owned = exchange(projected).reshape(2 * chips, rows, 4 * cols)
    order = chip_order()
    source = [2 * order.index(chip) + side for chip in range(chips) for side in range(2)]
    if cols != dim:
        owned = jnp.stack([owned[i] for i in source])
        source = list(range(heads))
        owned = owned.reshape(2 * chips, rows, 4, cols).transpose(1, 2, 0, 3).reshape(rows, 4, heads, dim)
        owned = owned.transpose(2, 0, 1, 3).reshape(heads, rows, 4 * dim)
    mixed, gates = call(
        functools.partial(mixer_body, source),
        [full, shape((3, heads * rows, dim), f32)],
        (owned, state, lower_bound.reshape(heads, dim), head_gain.reshape(1, dim)),
        12,
        scratch=[
            pltpu.VMEM((heads * rows, 4 * dim), f32),
            pltpu.VMEM((heads * rows, dim), f32),
            pltpu.VMEM((heads * rows, dim), f32),
        ],
    )
    mixer_cols = call(
        out_body, shape((chips, 2, half, cols), bf16), (exchange(mixed), w_out, out_cross), 6, scratch=rows_scratch
    )
    normed, middle = call(
        norm_body,
        [shape((half, width), bf16), shape((chips, rows, width), f32)],
        (all_tokens, exchange(mixer_cols), norm_ffn.reshape(1, width)),
        6,
        scratch=rows_scratch,
    )
    vmem = pl.BlockSpec(memory_space=pltpu.VMEM)
    keep, send, new_state = pl.pallas_call(
        expert_body,
        out_shape=[shape((chips, rows, width), f32), full, shape(state.shape, f32)],
        in_specs=[vmem] * 7,
        out_specs=[vmem, vmem, pl.BlockSpec(memory_space=pltpu.HBM)],
        scratch_shapes=[
            pltpu.VMEM((2 * half, width), bf16),
            pltpu.VMEM((2 * half, expert_gate.shape[1]), bf16),
            pltpu.VMEM(state.shape, f32),
            pltpu.SemaphoreType.DMA((heads,)),
        ],
        compiler_params=pltpu.CompilerParams(vmem_limit_bytes=14 * MIB),
        cost_estimate=pl.CostEstimate(flops=COST, bytes_accessed=0, transcendentals=0),
        name="experts",
    )(normed, swap(normed), expert_gate, expert_up, expert_down, gates, state)
    partials = call(add_body, full, (keep, swap(send)), 4)
    returned = exchange(partials)
    layer_out = call(
        functools.partial(final_body, group),
        shape((rows, width), bf16),
        (middle, returned, route_ids.T, route_weights.T),
        4,
        scratch=[pltpu.VMEM((8, LANES), f32)],
    )
    return (layer_out, new_state)


def solution(mesh):
    groups, size = mesh.shape["grp"], mesh.shape["ep"]
    split = Mesh(mesh.devices.reshape(groups, size // 2, 2), ("grp", *AXES))
    return jax.shard_map(
        body,
        mesh=split,
        in_specs=(
            P(("grp", *AXES), None),
            P(("grp", *AXES), None, None, None),
            P(("grp", *AXES), None),
            P(("grp", *AXES), None),
            P(),
            P(None, AXES),
            P(None, AXES),
            P(None, AXES),
            P(None, AXES),
            P(),
            P(),
            P(None, AXES),
            P(),
            P(None, AXES),
            P(None, AXES),
            P(AXES, None),
        ),
        out_specs=(P(("grp", *AXES), None), P(("grp", *AXES), None, None, None)),
        check_vma=False,
    )
```

```python
import functools

import jax
import jax.numpy as jnp
from jax import lax
from jax.experimental import pallas as pl
from jax.experimental.pallas import tpu as pltpu
from jax.sharding import Mesh
from jax.sharding import PartitionSpec as P

FF = 7168
EXPERTS = 4
LANES = 128
MIB = 1 << 20
COST = 10**10

epsilon = 1e-06
f32 = jnp.float32
bf16 = jnp.bfloat16


def call(body, outs, args, limit, spaces=None, scratch=(), flops=0, **kwargs):
    spaces = spaces or [pltpu.VMEM] * len(args)
    return pl.pallas_call(
        body,
        out_shape=outs,
        in_specs=[pl.BlockSpec(memory_space=space) for space in spaces],
        out_specs=jax.tree.map(lambda _: pl.BlockSpec(memory_space=pltpu.VMEM), outs),
        scratch_shapes=list(scratch),
        compiler_params=pltpu.CompilerParams(vmem_limit_bytes=limit * MIB),
        cost_estimate=pl.CostEstimate(flops=flops, bytes_accessed=0, transcendentals=0),
        **kwargs,
    )(*args)


AXES = ("chip", "core")


def chip_order():
    half = lax.axis_size("chip") // 2
    inward = [i // 2 if i % 2 == 0 else half - 1 - i // 2 for i in range(half)]
    return [2 * z + (lap ^ ((i ^ (i >> 1)) & 1)) for lap in range(2) for i, z in enumerate(inward)]


def my_place():
    chip = lax.axis_index("chip")
    place = jnp.int32(0)
    for i, other in enumerate(chip_order()):
        place = jnp.where(chip == other, i, place)
    return place


def lines():
    return [[2 * chip + (line ^ chip % 2) for chip in chip_order()] for line in range(2)]


def exchange(chunks):
    return lax.all_to_all(chunks, AXES, split_axis=0, concat_axis=0, axis_index_groups=lines(), tiled=True)


def swap(values):
    return lax.ppermute(values, "core", [(0, 1), (1, 0)])


def rms(values):
    return values * lax.rsqrt(jnp.mean(values * values, axis=-1, keepdims=True) + epsilon)


def unpack(source, target):
    count, rows = source.shape[0], source.shape[1]
    for i in range(count):
        target[i * rows : (i + 1) * rows, :] = source[i].astype(f32)


def mark_body(out_ref):
    out_ref[...] = jnp.zeros(out_ref.shape, out_ref.dtype)


def spread_body(rows_ref, mark_ref, out_ref):
    for i in range(out_ref.shape[0]):
        out_ref[i] = rows_ref[...]


def project_body(all_ref, gain_ref, *refs):
    weights, (out_ref, rows_ref) = refs[:8], refs[8:]
    rows, cols = all_ref.shape[1], weights[0].shape[1]
    core = lax.axis_index("core")
    unpack(all_ref, rows_ref)
    normed = (rms(rows_ref[...]) * gain_ref[...]).astype(bf16)
    for i, w_ref in enumerate(weights):
        p, cross = divmod(i, 2)
        side = 1 - core if cross else core
        product = jnp.dot(normed, w_ref[...], preferred_element_type=f32)
        for chip in range(all_ref.shape[0]):
            block = product[chip * rows : (chip + 1) * rows, :].astype(bf16)
            out_ref[chip, side, :, p * cols : (p + 1) * cols] = block


def thirds(values):
    first = values.astype(bf16).astype(f32)
    second = (values - first).astype(bf16).astype(f32)
    return first, second, (values - first - second).astype(bf16).astype(f32)


def chooser(count, dim):
    shape = (3 * count, count * dim)
    row, column = lax.broadcasted_iota(jnp.int32, shape, 0), lax.broadcasted_iota(jnp.int32, shape, 1)
    return (row % count == column // dim).astype(f32)


def mixer_body(source, owned_ref, state_ref, bound_ref, gain_ref, out_ref, gates_ref, raw_ref, bounds_ref, read_ref):
    heads, rows = owned_ref.shape[0], owned_ref.shape[1]
    dim = bound_ref.shape[1]
    for h in range(heads):
        raw_ref[h * rows : (h + 1) * rows, :] = owned_ref[source[h]].astype(f32)
        bounds_ref[h * rows : (h + 1) * rows, :] = jnp.broadcast_to(bound_ref[h : h + 1, :], (rows, dim))
    bound = bounds_ref[...]
    query_raw, forget_raw, input_raw, gate_raw = (raw_ref[:, p * dim : (p + 1) * dim] for p in range(4))
    decay = bound + (1.0 - bound) * jax.nn.sigmoid(forget_raw)
    key_vec = (1.0 - bound) * jax.nn.sigmoid(-forget_raw)
    query_vec = query_raw * jax.nn.sigmoid(query_raw) * dim ** (-0.5)
    gates_ref[0] = decay
    gates_ref[1] = key_vec
    gates_ref[2] = input_raw
    weights = thirds(query_vec * decay)
    take = min(16, heads * rows)
    chosen = chooser(take, dim).astype(bf16)
    for start in range(0, heads * rows, take):
        columns = jnp.concatenate([part[start : start + take, :] for part in weights], axis=0).T
        wide = jnp.dot(columns.astype(bf16), chosen, preferred_element_type=f32)
        for j in range(take):
            h, t = divmod(start + j, rows)
            product = wide[:, j * dim : (j + 1) * dim] * state_ref[t, h]
            read_ref[start + j : start + j + 1, :] = jnp.sum(product, axis=0, keepdims=True)
    read = read_ref[...] + jnp.sum(query_vec * key_vec, axis=-1, keepdims=True) * input_raw
    mixed = rms(read) * gain_ref[...] * (gate_raw * jax.nn.sigmoid(gate_raw))
    for h in range(heads):
        block = mixed[h * rows : (h + 1) * rows, :].astype(bf16)
        for i in range(out_ref.shape[0]):
            out_ref[i, :, h * dim : (h + 1) * dim] = block


def out_body(all_ref, own_ref, cross_ref, out_ref, rows_ref):
    core = lax.axis_index("core")
    unpack(all_ref, rows_ref)
    mixed = rows_ref[...].astype(bf16)
    for side, w_ref in ((core, own_ref), (1 - core, cross_ref)):
        block = jnp.dot(mixed, w_ref[...], preferred_element_type=f32).astype(bf16)
        for i in range(out_ref.shape[0]):
            out_ref[i, side] = block


def norm_body(tokens_ref, mixer_ref, gain_ref, normed_ref, middle_ref, rows_ref):
    rows, cols = middle_ref.shape[1], mixer_ref.shape[3]
    unpack(tokens_ref, rows_ref)
    for place, chip in enumerate(chip_order()):
        for side in range(2):
            part = slice((2 * chip + side) * cols, (2 * chip + side + 1) * cols)
            rows_ref[:, part] = rows_ref[:, part] + mixer_ref[place, side].astype(f32)
    normed_ref[...] = (rms(rows_ref[...]) * gain_ref[...]).astype(bf16)
    for chip in range(middle_ref.shape[0]):
        middle_ref[chip] = rows_ref[chip * rows : (chip + 1) * rows, :]


def expert_body(
    mine_ref,
    other_ref,
    gate_ref,
    up_ref,
    down_ref,
    gates_ref,
    state_ref,
    keep_ref,
    send_ref,
    new_ref,
    normed_ref,
    hidden_ref,
    held_ref,
    sems,
):
    chips, rows = keep_ref.shape[:2]
    half = mine_ref.shape[0]
    hidden_cols, width = gate_ref.shape[1], down_ref.shape[1]
    seqs, heads, dim = state_ref.shape[:3]
    step_heads = max(1, 8 // seqs)
    take, groups = step_heads * seqs, heads // step_heads
    step = 2 * LANES
    blocks = [pl.ds(i, min(step, hidden_cols - i)) for i in range(0, hidden_cols, step)]
    parts = [pl.ds(i, min(step, width - i)) for i in range(0, width, step)]
    normed_ref[:half, :] = mine_ref[...]
    normed_ref[half:, :] = other_ref[...]
    normed = normed_ref[...]
    copies = []

    chosen = chooser(take, dim)

    def renew(g):
        group = slice(g * take, (g + 1) * take)
        decay, key_vec, value = gates_ref[0, group, :].T, thirds(gates_ref[1, group, :]), gates_ref[2, group, :]
        columns = jnp.concatenate(key_vec, axis=0).T.astype(bf16)
        values = jnp.concatenate([jnp.concatenate([value] * 3, axis=0)] * take, axis=1) * chosen
        outer = jnp.dot(columns, values.astype(bf16), preferred_element_type=f32)
        for j in range(take):
            h, t = divmod(g * take + j, seqs)
            held_ref[t, h] = decay[:, j : j + 1] * state_ref[t, h] + outer[:, j * dim : (j + 1) * dim]
        part = pl.ds(g * step_heads, step_heads)
        copies.append(pltpu.make_async_copy(held_ref.at[:, part], new_ref.at[:, part], sems.at[g]))
        copies[-1].start()

    for i, block in enumerate(blocks):
        gate_act = jnp.dot(normed, gate_ref[:, block], preferred_element_type=f32)
        up_act = jnp.dot(normed, up_ref[:, block], preferred_element_type=f32)
        for g in range(i * groups // len(blocks), (i + 1) * groups // len(blocks)):
            renew(g)
        hidden_ref[:, block] = (gate_act * jax.nn.sigmoid(gate_act) * up_act).astype(bf16)
    hidden = hidden_ref[...]
    for part in parts:
        product = jnp.dot(hidden, down_ref[:, part], preferred_element_type=f32)
        for side, out_ref in enumerate((keep_ref, send_ref)):
            for chip in range(chips):
                start = (side * chips + chip) * rows
                out_ref[chip, :, part] = product[start : start + rows, :].astype(out_ref.dtype)
    for copy in copies:
        copy.wait()


def add_body(keep_ref, came_ref, out_ref):
    out_ref[...] = (keep_ref[...] + came_ref[...].astype(f32)).astype(bf16)


def final_body(group, middle_ref, returned_ref, ids_ref, weights_ref, out_ref, shares_ref):
    total = middle_ref[my_place()]
    rows = total.shape[0]
    ids, weights = ids_ref[...], weights_ref[...].astype(f32)
    shares_ref[...] = jnp.zeros(shares_ref.shape, f32)
    for e in range(EXPERTS):
        shares_ref[e : e + 1, :rows] = jnp.sum(jnp.where(ids == e, weights, 0.0), axis=0, keepdims=True)
    shares = shares_ref[...].T
    for e in range(EXPERTS):
        share = shares[:rows, e : e + 1]
        places = [place for place, chip in enumerate(chip_order()) if chip // group == e]
        summed = returned_ref[places[0]].astype(f32)
        for place in places[1:]:
            summed = summed + returned_ref[place].astype(f32)
        total = total + share * summed
    out_ref[...] = total.astype(bf16)


def body(
    tokens,
    state,
    route_ids,
    route_weights,
    norm_mix,
    w_query,
    w_forget,
    w_input,
    w_gate,
    lower_bound,
    head_gain,
    w_out,
    norm_ffn,
    expert_gate,
    expert_up,
    expert_down,
):
    rows, width = tokens.shape
    heads, dim = state.shape[1], state.shape[2]
    chips = lax.axis_size("chip")
    cols = w_query.shape[1]
    half = chips * rows
    group = FF // expert_gate.shape[1] // 2
    shape = jax.ShapeDtypeStruct
    full = shape((chips, rows, width), bf16)
    rows_scratch = [pltpu.VMEM((half, width), f32)]

    weights = []
    for weight in (w_query, w_forget, w_input, w_gate, w_out):
        weights += [weight, swap(weight)]
    mark = call(mark_body, shape((8, LANES), f32), (), 1, flops=COST)
    sent = call(spread_body, full, (tokens, mark), 4, flops=COST)
    all_tokens = exchange(sent)
    all_tokens, out_cross = lax.optimization_barrier((all_tokens, weights[9]))
    projected = call(
        project_body,
        shape((chips, 2, rows, 4 * cols), bf16),
        (all_tokens, norm_mix.reshape(1, width), *weights[:8]),
        8,
        scratch=rows_scratch,
    )
    owned = exchange(projected).reshape(2 * chips, rows, 4 * cols)
    order = chip_order()
    source = [2 * order.index(chip) + side for chip in range(chips) for side in range(2)]
    if cols != dim:
        owned = jnp.stack([owned[i] for i in source])
        source = list(range(heads))
        owned = owned.reshape(2 * chips, rows, 4, cols).transpose(1, 2, 0, 3).reshape(rows, 4, heads, dim)
        owned = owned.transpose(2, 0, 1, 3).reshape(heads, rows, 4 * dim)
    mixed, gates = call(
        functools.partial(mixer_body, source),
        [full, shape((3, heads * rows, dim), f32)],
        (owned, state, lower_bound.reshape(heads, dim), head_gain.reshape(1, dim)),
        12,
        scratch=[
            pltpu.VMEM((heads * rows, 4 * dim), f32),
            pltpu.VMEM((heads * rows, dim), f32),
            pltpu.VMEM((heads * rows, dim), f32),
        ],
    )
    mixer_cols = call(
        out_body, shape((chips, 2, half, cols), bf16), (exchange(mixed), w_out, out_cross), 6, scratch=rows_scratch
    )
    normed, middle = call(
        norm_body,
        [shape((half, width), bf16), shape((chips, rows, width), f32)],
        (all_tokens, exchange(mixer_cols), norm_ffn.reshape(1, width)),
        6,
        scratch=rows_scratch,
    )
    vmem = pl.BlockSpec(memory_space=pltpu.VMEM)
    keep, send, new_state = pl.pallas_call(
        expert_body,
        out_shape=[shape((chips, rows, width), f32), full, shape(state.shape, f32)],
        in_specs=[vmem] * 7,
        out_specs=[vmem, vmem, pl.BlockSpec(memory_space=pltpu.HBM)],
        scratch_shapes=[
            pltpu.VMEM((2 * half, width), bf16),
            pltpu.VMEM((2 * half, expert_gate.shape[1]), bf16),
            pltpu.VMEM(state.shape, f32),
            pltpu.SemaphoreType.DMA((heads,)),
        ],
        compiler_params=pltpu.CompilerParams(vmem_limit_bytes=14 * MIB),
        cost_estimate=pl.CostEstimate(flops=COST, bytes_accessed=0, transcendentals=0),
        name="experts",
    )(normed, swap(normed), expert_gate, expert_up, expert_down, gates, state)
    partials = call(add_body, full, (keep, swap(send)), 4)
    returned = exchange(partials)
    layer_out = call(
        functools.partial(final_body, group),
        shape((rows, width), bf16),
        (middle, returned, route_ids.T, route_weights.T),
        4,
        scratch=[pltpu.VMEM((8, LANES), f32)],
    )
    return (layer_out, new_state)


def solution(mesh):
    groups, size = mesh.shape["grp"], mesh.shape["ep"]
    split = Mesh(mesh.devices.reshape(groups, size // 2, 2), ("grp", *AXES))
    return jax.shard_map(
        body,
        mesh=split,
        in_specs=(
            P(("grp", *AXES), None),
            P(("grp", *AXES), None, None, None),
            P(("grp", *AXES), None),
            P(("grp", *AXES), None),
            P(),
            P(None, AXES),
            P(None, AXES),
            P(None, AXES),
            P(None, AXES),
            P(),
            P(),
            P(None, AXES),
            P(),
            P(None, AXES),
            P(None, AXES),
            P(AXES, None),
        ),
        out_specs=(P(("grp", *AXES), None), P(("grp", *AXES), None, None, None)),
        check_vma=False,
    )
```
